32 devices in a mesh: sp: 8 (over z, y), tp: 4 (over x, core).
Axes of the slice: x: 2, y: 2, z: 4, core: 2. Of those that a mesh axis runs over, the one named last changes fastest.
Arguments:
- arriving_hidden_state: bfloat16 [8192, 2048], P(('sp', 'tp')), may hold values from -6 to 6
- former_request_vectors: bfloat16 [8192, 1024], P('sp', 'tp'), may hold values from -6 to 6
- former_match_vectors: bfloat16 [8192, 1024], P('sp', 'tp'), may hold values from -6 to 6
- latter_request_vectors: bfloat16 [8192, 512], P('sp', 'tp'), may hold values from -6 to 6
- latter_match_vectors: bfloat16 [8192, 512], P('sp', 'tp'), may hold values from -6 to 6
- stored_vectors_both: bfloat16 [8192, 2, 1024], P('sp', None, 'tp'), may hold values from -6 to 6
- closing_valve_operands: bfloat16 [8192, 2, 1024], P('sp', None, 'tp'), may hold values from -6 to 6
- update_level_before_squash: bfloat16 [2, 8, 8192], P(None, 'tp', 'sp'), may hold values from -4 to -3
- fading_data_input: float32 [2, 8, 8192], P(None, 'tp', 'sp'), may hold values from -5.5 to 5.5
- sparse_fading_boost: float32 [2, 8, 8192], P(None, 'tp', 'sp'), may hold values from -2 to 0, as said below
- unitwise_fading_loglevel: float32 [2, 8], P(None, 'tp'), as said below
- fading_constant_term: float32 [2, 8], P(None, 'tp'), may hold values from -1 to 1
- unitwise_normalizer_coef: float32 [128], replicated, may hold values from 0.1 to 1.9
- emission_map_weights: bfloat16 [2048, 2048], replicated, may hold values from -0.125 to 0.125
- channel_normalizer_coef: float32 [2048], replicated, may hold values from 0.1 to 1.9
- switching_channel_map: bfloat16 [2048, 6144], P('sp', 'tp'), may hold values from -0.125 to 0.125
- broadening_channel_map: bfloat16 [2048, 6144], P('sp', 'tp'), may hold values from -0.125 to 0.125
- timewise_convolve_tapvalues: bfloat16 [3, 2, 6144], P(None, None, 'tp'), may hold values from -3.5 to 3.5
- narrowing_map_weights_in: bfloat16 [2048, 6144], P('sp', 'tp'), may hold values from -0.078125 to 0.078125
Outputs:
- mixed: bfloat16 [8192, 2048], P(('sp', 'tp'))
The draws below stay inside these ranges and needn't reach their ends.
Inputs may be any that keep to these rules, and one draw needn't show every extreme that they name: `unitwise_fading_loglevel`: each entry is the logarithm of a per-position rate between 0.2 / 8192 and 2 / 64. `sparse_fading_boost`: zero except at three or fewer positions of the sequence.
All inputs are finite; a program needn't handle non-finite values.
Results may differ from the reference program's by a relative error of at most 0.015.
Values may be sent and summed in bfloat16 or wider, within the bound.
A program may use at most 128 MiB of HBM per device.

```python
import jax
import jax.numpy as jnp
from jax import lax

MODEL_WIDTH = 2048
ATTN_UNITS = 8
DK_ONE = 128
DK_TWO = 64
VALUE_DIM = 128
FF = 6144
SPAN = 64
TAPS = 3
TOK_DEV = 1024
STEP_TOTAL = 8192
VW = 2048
N_TP = 4


def drawn_keys(key, column_count):
    direction_key, jitter_key = jax.random.split(key)
    directions = jax.random.normal(direction_key, (STEP_TOTAL // SPAN, column_count), jnp.float32)
    repeated = jnp.repeat(directions, SPAN, axis=0)
    jitter = jax.random.normal(jitter_key, (STEP_TOTAL, column_count), jnp.float32)
    jitter_scale = 0.2
    return jnp.clip(repeated + jitter_scale * jitter, -6.0, 6.0).astype(jnp.bfloat16)


def draw_former_match_vectors(key, part):
    return drawn_keys(jax.random.fold_in(key, 71), ATTN_UNITS * DK_ONE)


def draw_latter_match_vectors(key, part):
    return drawn_keys(jax.random.fold_in(key, 79), ATTN_UNITS * DK_TWO)


def draw_update_level_before_squash(key, part):
    drawn = jax.random.uniform(jax.random.fold_in(key, 53), (2, ATTN_UNITS, STEP_TOTAL), jnp.float32, -4.0, -3.0)
    return drawn.astype(jnp.bfloat16)


def draw_fading_data_input(key, part):
    noise_key, shift_key = jax.random.split(jax.random.fold_in(key, 11))
    noise_draw = jax.random.truncated_normal(noise_key, -4.0, 4.0, (2, ATTN_UNITS, STEP_TOTAL), jnp.float32)
    offsets = jax.random.uniform(shift_key, (2, ATTN_UNITS, STEP_TOTAL // TOK_DEV), jnp.float32, -1.5, 1.5)
    offset_rows = jnp.repeat(offsets, TOK_DEV, axis=2)
    return noise_draw + offset_rows


def draw_sparse_fading_boost(key, part):
    position_random_key, size_key = jax.random.split(jax.random.fold_in(key, 23))
    spike_positions = jax.random.randint(position_random_key, (3,), 0, STEP_TOTAL)
    kept_share = jax.random.uniform(size_key, (2, ATTN_UNITS, 3), jnp.float32, 0.55, 0.8)
    position_hits = (jnp.arange(STEP_TOTAL)[None, :] == spike_positions[:, None]).astype(jnp.float32)
    return jnp.einsum('ghb,bs->ghs', jnp.log(kept_share), position_hits)


def draw_unitwise_fading_loglevel(key, part):
    pick_key, fast_key, slow_key = jax.random.split(jax.random.fold_in(key, 37), 3)
    fast_share = 0.5
    fast_mask = jax.random.uniform(pick_key, (2, ATTN_UNITS), jnp.float32) < fast_share
    fast_rate = jax.random.uniform(fast_key, (2, ATTN_UNITS), jnp.float32, 1.0, 2.0) / SPAN
    slow_rate = jax.random.uniform(slow_key, (2, ATTN_UNITS), jnp.float32, 0.2, 0.4) / STEP_TOTAL
    return jnp.log(jnp.where(fast_mask, fast_rate, slow_rate))


def level_of(key, dims, cuts, smallest, high):
    loudness, own = 1.0, jax.random.fold_in(key, 6)
    for axis_at, shards_of in cuts:
        heights = jnp.exp(jax.random.uniform(jax.random.fold_in(own, axis_at), (shards_of,), jnp.float32, smallest / len(cuts), high / len(cuts)))
        loudness = loudness * jnp.repeat(heights, dims[axis_at] // shards_of).reshape([-1 if axis == axis_at else 1 for axis in range(len(dims))])
    return loudness


def gaussian(rng, shape, scale, most, shards=(), kind=jnp.bfloat16):
    entries = jax.random.normal(rng, shape, jnp.float32) * scale
    if len(shards) > 0:
        entries = level_of(rng, shape, shards, -0.22, 0.18) * entries
    return jnp.clip(entries, min=-most, max=most).astype(kind)


def setup_inputs(seed: int = 0) -> dict:
    streams_of = jax.random.split(jax.random.key(seed), 20)
    return {
        "arriving_hidden_state": gaussian(streams_of[0], (STEP_TOTAL, MODEL_WIDTH), 1.0, 6.0, ((0, 32),)),
        "former_request_vectors": gaussian(streams_of[1], (STEP_TOTAL, ATTN_UNITS * DK_ONE), 1.0, 6.0, ((0, 8), (1, 4))),
        "former_match_vectors": draw_former_match_vectors(jax.random.fold_in(streams_of[19], 71), 0),
        "latter_request_vectors": gaussian(streams_of[3], (STEP_TOTAL, ATTN_UNITS * DK_TWO), 1.0, 6.0, ((0, 8), (1, 4))),
        "latter_match_vectors": draw_latter_match_vectors(jax.random.fold_in(streams_of[19], 71), 0),
        "stored_vectors_both": gaussian(streams_of[5], (STEP_TOTAL, 2, ATTN_UNITS * VALUE_DIM), 1.0, 6.0, ((0, 8), (2, 4))),
        "closing_valve_operands": gaussian(streams_of[6], (STEP_TOTAL, 2, ATTN_UNITS * VALUE_DIM), 1.0, 6.0, ((0, 8), (2, 4))),
        "update_level_before_squash": draw_update_level_before_squash(jax.random.fold_in(streams_of[19], 71), 0),
        "fading_data_input": draw_fading_data_input(jax.random.fold_in(streams_of[19], 71), 0),
        "sparse_fading_boost": draw_sparse_fading_boost(jax.random.fold_in(streams_of[19], 71), 0),
        "unitwise_fading_loglevel": draw_unitwise_fading_loglevel(jax.random.fold_in(streams_of[19], 71), 0),
        "fading_constant_term": jnp.clip(jax.random.uniform(streams_of[11], (2, ATTN_UNITS), jnp.float32, -1.0, 1.0) * level_of(streams_of[11], (2, ATTN_UNITS), ((1, 4),), -0.4, 0.0), -1.0, 1.0),
        "unitwise_normalizer_coef": jnp.clip(1.0 + 0.18 * jax.random.normal(streams_of[12], (VALUE_DIM,), jnp.float32), 0.1, 1.9),
        "emission_map_weights": gaussian(streams_of[13], (VW, MODEL_WIDTH), VW ** -0.5, 0.125),
        "channel_normalizer_coef": jnp.clip(1.0 + 0.18 * jax.random.normal(streams_of[14], (MODEL_WIDTH,), jnp.float32), 0.1, 1.9),
        "switching_channel_map": gaussian(streams_of[15], (MODEL_WIDTH, FF), MODEL_WIDTH ** -0.5, 0.125, ((0, 8), (1, 4))),
        "broadening_channel_map": gaussian(streams_of[16], (MODEL_WIDTH, FF), MODEL_WIDTH ** -0.5, 0.125, ((0, 8), (1, 4))),
        "timewise_convolve_tapvalues": gaussian(streams_of[17], (TAPS, 2, FF), TAPS ** -0.5, 3.5, ((2, 4),)),
        "narrowing_map_weights_in": gaussian(streams_of[18], (MODEL_WIDTH, FF), FF ** -0.5, 0.078125, ((0, 8), (1, 4))),
    }


EPSILON = 1e-06
PRECISE = lax.Precision.HIGHEST

def unit_rows(matrix):
    return matrix * lax.rsqrt(lax.optimization_barrier(jnp.sum(matrix * matrix, axis=-1, keepdims=True)) + EPSILON)

def heads_first(matrix, head_count):
    row_count = matrix.shape[0]
    return matrix.reshape(row_count, head_count, -1).astype(jnp.float32).transpose(1, 0, 2)

def block_terms(queries, key_rows, value_rows, beta_rate, gate_logarithms):
    head_count, length, key_size = queries.shape
    num_blocks = length // SPAN
    queries = queries.reshape(head_count, num_blocks, SPAN, -1)
    key_rows = key_rows.reshape(head_count, num_blocks, SPAN, -1)
    value_rows = value_rows.reshape(head_count, num_blocks, SPAN, -1)
    beta_rate = beta_rate.reshape(head_count, num_blocks, SPAN)
    cum_gates = jnp.cumsum(gate_logarithms.reshape(head_count, num_blocks, SPAN), axis=-1)
    row_pos = lax.broadcasted_iota(jnp.int32, (SPAN, SPAN), 0)
    col_pos = lax.broadcasted_iota(jnp.int32, (SPAN, SPAN), 1)
    causal = row_pos >= col_pos
    strict = row_pos > col_pos
    decay = jnp.exp(jnp.where(causal, cum_gates[..., :, None] - cum_gates[..., None, :], -jnp.inf))
    key_beta = key_rows * beta_rate[..., None]
    lower = jnp.where(strict, jnp.einsum('hncd,hnsd->hncs', key_beta, key_rows, precision=PRECISE) * decay, 0.0)
    right_side = jnp.concatenate([value_rows * beta_rate[..., None], key_beta * jnp.exp(cum_gates)[..., None]], axis=-1)
    unit_mat = jnp.eye(SPAN, dtype=lower.dtype)
    solved = lax.linalg.triangular_solve(lower + unit_mat, right_side, left_side=True, lower=True, unit_diagonal=True)
    value_size = value_rows.shape[-1]
    u_values = solved[..., :value_size]
    w_keys = solved[..., value_size:]
    intra = jnp.einsum('hncd,hnsd->hncs', queries, key_rows, precision=PRECISE) * decay
    key_decayed = key_rows * jnp.exp(cum_gates[..., -1:] - cum_gates)[..., None]
    return (queries, u_values, w_keys, intra, key_decayed, cum_gates)

def run_blocks(increment_list, initial_memory):

    def advance(state_mat, inputs):
        query_blk, u_blk, w_blk, intra_blk, kdec_blk, cum_blk = inputs
        fresh = u_blk - jnp.einsum('hcd,hde->hce', w_blk, state_mat, precision=PRECISE)
        output = jnp.einsum('hcd,hde->hce', query_blk * jnp.exp(cum_blk)[..., None], state_mat, precision=PRECISE)
        output = output + jnp.einsum('hcs,hse->hce', intra_blk, fresh, precision=PRECISE)
        state_mat = state_mat * jnp.exp(cum_blk[:, -1])[:, None, None]
        state_mat = state_mat + jnp.einsum('hcd,hce->hde', kdec_blk, fresh, precision=PRECISE)
        return (state_mat, output)
    moved = tuple((jnp.moveaxis(member, 1, 0) for member in increment_list))
    _, outputs = lax.scan(advance, initial_memory, moved)
    head_count = outputs.shape[1]
    return jnp.moveaxis(outputs, 0, 1).reshape(head_count, -1, outputs.shape[-1])

def team_parts(asker_weights, lookup_weights, value_matrix, correction_draw, decay_draw, spike_draw, decay_logarithm, bias_vector):
    head_count = decay_logarithm.shape[0]
    queries = heads_first(asker_weights, head_count)
    key_size = queries.shape[-1]
    queries = unit_rows(queries) * key_size ** (-0.5)
    key_rows = unit_rows(heads_first(lookup_weights, head_count))
    value_rows = heads_first(value_matrix, head_count)
    beta_rate = jax.nn.sigmoid(correction_draw.astype(jnp.float32))
    gate_logarithms = -jnp.exp(decay_logarithm)[:, None] * jax.nn.softplus(decay_draw + bias_vector[:, None]) + spike_draw
    return block_terms(queries, key_rows, value_rows, beta_rate, gate_logarithms)

def completed_attn_units(increment_list, initial_memory, gate_cols, unitwise_normalizer_coef):
    outputs = run_blocks(increment_list, initial_memory)
    head_count = outputs.shape[0]
    gates_in = heads_first(gate_cols, head_count)
    scaled = outputs * lax.rsqrt(lax.optimization_barrier(jnp.mean(outputs * outputs, axis=-1, keepdims=True)) + EPSILON) * unitwise_normalizer_coef
    scaled = scaled * jax.nn.silu(gates_in)
    return scaled.transpose(1, 0, 2).reshape(outputs.shape[1], -1).astype(jnp.bfloat16)

def causal_taps(low_rows, taps_col):
    padded = jnp.concatenate([jnp.zeros((TAPS - 1, low_rows.shape[1]), low_rows.dtype), low_rows], axis=0)
    length = low_rows.shape[0]
    total = taps_col[0] * padded[0:length]
    for tap_index in range(1, TAPS):
        total = total + taps_col[tap_index] * padded[tap_index:tap_index + length]
    return total

def reference(arriving_hidden_state, former_request_vectors, former_match_vectors, latter_request_vectors, latter_match_vectors, stored_vectors_both, closing_valve_operands, update_level_before_squash, fading_data_input, sparse_fading_boost, unitwise_fading_loglevel, fading_constant_term, unitwise_normalizer_coef, emission_map_weights, channel_normalizer_coef, switching_channel_map, broadening_channel_map, timewise_convolve_tapvalues, narrowing_map_weights_in):
    combined_attn_units = []
    pairs = ((former_request_vectors, former_match_vectors), (latter_request_vectors, latter_match_vectors))
    for cohort_ordinal in range(2):
        asker_weights, lookup_weights = pairs[cohort_ordinal]
        increment_list = team_parts(asker_weights, lookup_weights, stored_vectors_both[:, cohort_ordinal], update_level_before_squash[cohort_ordinal], fading_data_input[cohort_ordinal], sparse_fading_boost[cohort_ordinal], unitwise_fading_loglevel[cohort_ordinal], fading_constant_term[cohort_ordinal])
        key_size = increment_list[0].shape[-1]
        head_count = unitwise_fading_loglevel.shape[1]
        initial_memory = jnp.zeros((head_count, key_size, stored_vectors_both.shape[-1] // head_count), jnp.float32)
        combined_attn_units.append(completed_attn_units(increment_list, initial_memory, closing_valve_operands[:, cohort_ordinal], unitwise_normalizer_coef))
    linear_attend = jnp.stack(combined_attn_units, axis=1)
    token_slices = linear_attend.shape[0]
    skip_stream = arriving_hidden_state.astype(jnp.float32) + jnp.dot(linear_attend.reshape(token_slices, -1).astype(jnp.float32), emission_map_weights.astype(jnp.float32), preferred_element_type=jnp.float32)
    normed = (skip_stream * lax.rsqrt(lax.optimization_barrier(jnp.mean(skip_stream * skip_stream, axis=-1, keepdims=True)) + EPSILON) * channel_normalizer_coef).astype(jnp.bfloat16)
    gate_low = jnp.dot(normed.astype(jnp.float32), switching_channel_map.astype(jnp.float32), preferred_element_type=jnp.float32).astype(jnp.bfloat16)
    up_low = jnp.dot(normed.astype(jnp.float32), broadening_channel_map.astype(jnp.float32), preferred_element_type=jnp.float32).astype(jnp.bfloat16)
    taps = timewise_convolve_tapvalues.astype(jnp.float32)
    gate_conv = causal_taps(gate_low, taps[:, 0])
    up_conv = causal_taps(up_low, taps[:, 1])
    hidden = (jax.nn.silu(gate_conv) * up_conv).astype(jnp.bfloat16)
    shard_width = hidden.shape[1] // N_TP
    down_sum = jnp.zeros(skip_stream.shape, jnp.float32)
    for shard_index in range(N_TP):
        lower_col = shard_index * shard_width
        partial_value = lax.dot_general(hidden[:, lower_col:lower_col + shard_width].astype(jnp.float32), narrowing_map_weights_in[:, lower_col:lower_col + shard_width].astype(jnp.float32), (((1,), (1,)), ((), ())), preferred_element_type=jnp.float32)
        down_sum = down_sum + lax.optimization_barrier(partial_value.astype(jnp.bfloat16)).astype(jnp.float32)
    return (skip_stream + down_sum).astype(jnp.bfloat16)
```

```python
import functools

import jax
import jax.numpy as jnp
from jax import lax
from jax.experimental import pallas as pl
from jax.experimental.pallas import tpu as pltpu
from jax.sharding import PartitionSpec as P

TAPS = 3
CHUNK = 128
BASE = 16
LANES = 128
EDGE = 16
UP, DOWN, ACROSS = 0, 1, 2

EPSILON = 1e-06
F32 = jnp.float32
BF16 = jnp.bfloat16
MESH = pl.DeviceIdType.MESH


def mm(a, b):
    return jnp.dot(a, b, preferred_element_type=F32)


def mm_nt(a, b):
    return lax.dot_general(a, b, (((1,), (1,)), ((), ())), preferred_element_type=F32)


def attend_heads(first, it, q_ref, k_ref, v_ref, cum_ref, gb_ref, heads, pm_ref, h0_ref, run_ref, last_ref):
    n = v_ref.shape[1] // CHUNK
    rows = lax.broadcasted_iota(jnp.int32, (CHUNK, CHUNK), 0)
    cols = lax.broadcasted_iota(jnp.int32, (CHUNK, CHUNK), 1)
    causal = rows >= cols
    eye = (rows == cols).astype(F32)
    lane = lax.broadcasted_iota(jnp.int32, (1, LANES), 1)
    narrow = it >= first
    other = jnp.maximum(it - first, 0)
    tile = jnp.where(narrow, first + other // 2, it)
    own = (lane // (LANES // 2) == other % 2) | jnp.logical_not(narrow)
    keep = jnp.where(own, 1.0, 0.0)
    diag = jnp.where(own, eye, 0.0)
    scale = jnp.where(narrow, (LANES // 2) ** -0.5, LANES ** -0.5)
    R = range(n)
    at = [pl.ds(c * CHUNK, CHUNK) for c in R]
    ks, qs, vs, low, intra, grown, fall, total, betas = ([None] * n for _ in range(9))
    for c in R:
        q = q_ref[tile, at[c], :].astype(F32) * keep
        k = k_ref[tile, at[c], :].astype(F32) * keep
        q = q * (lax.rsqrt(jnp.sum(q * q, axis=-1, keepdims=True) + EPSILON) * scale)
        k = k * lax.rsqrt(jnp.sum(k * k, axis=-1, keepdims=True) + EPSILON)
        cum = cum_ref[it, :, at[c]]
        beta = cum_ref[heads + it, :, at[c]]
        crow = jnp.broadcast_to(cum, (CHUNK, CHUNK))
        ccol = crow.T
        bcol = jnp.broadcast_to(beta, (CHUNK, CHUNK)).T
        total[c] = crow[:, CHUNK - 1:]
        decay = jnp.exp(jnp.where(causal, ccol - crow, -1e30))
        grown[c] = jnp.exp(ccol)
        kb = k.astype(BF16)
        kbeta = k * bcol
        both = mm_nt(jnp.concatenate([kbeta.astype(BF16), q.astype(BF16)], axis=0), kb)
        low[c] = jnp.where(rows > cols, both[:CHUNK] * decay, 0.0)
        intra[c] = (both[CHUNK:] * decay).astype(BF16)
        fall[c] = (k.T * jnp.exp(crow[:, CHUNK-1:] - crow)).astype(BF16)
        ks[c] = (kbeta * grown[c]).astype(BF16)
        vs[c] = (v_ref[it, at[c], :].astype(F32) * bcol).astype(BF16)
        qs[c] = q * grown[c]
    inner = (rows // BASE) == (cols // BASE)
    power = [jnp.where(inner, low[c], 0.0) for c in R]
    inv = [eye - power[c] for c in R]
    power = [p.astype(BF16) for p in power]
    size = 2
    while size < BASE:
        power = [mm(p, p).astype(BF16) for p in power]
        inv = [i + mm(i.astype(BF16), p) for i, p in zip(inv, power)]
        size *= 2
    block = BASE
    while block < CHUNK:
        here = ((rows // (2 * block)) == (cols // (2 * block))) & ((rows // block) != (cols // block))
        invb = [i.astype(BF16) for i in inv]
        half = [mm(invb[c], jnp.where(here, low[c], 0.0).astype(BF16)).astype(BF16) for c in R]
        inv = [inv[c] - mm(half[c], invb[c]) for c in R]
        block *= 2
    solved = [mm(inv[c].astype(BF16), jnp.concatenate([vs[c], ks[c]], axis=-1)).astype(BF16) for c in R]
    out = [mm(jnp.concatenate([fall[c], intra[c]], axis=0), solved[c]) for c in R]
    for c in R:
        h0_ref[it, at[c], :] = out[c][CHUNK:, :LANES]
        pm_ref[it, at[c], :] = (qs[c] - out[c][CHUNK:, LANES:]).astype(BF16)
    run = jnp.concatenate([jnp.zeros((LANES, LANES), F32), diag], axis=-1)
    for c in R:
        run_ref[it, c] = run.astype(BF16)
        cmap = (jnp.exp(total[c]) * diag - out[c][:CHUNK, LANES:]).astype(BF16)
        nxt = mm(cmap, run.astype(BF16))
        run = jnp.concatenate([nxt[:, :LANES] + out[c][:CHUNK, :LANES], nxt[:, LANES:]], axis=-1)
    last_ref[it] = run.astype(BF16)


def nearest(ring, place, rank):
    found = 0
    for here in range(ring):
        table = sorted(range(ring), key=lambda other: (abs(other - here), other))
        found = found + jnp.where(place == here, table[rank], 0)
    return found


def step_kernel(
    first,
    q1_ref, k1_ref, q2_ref, k2_ref, v_ref, valve_ref, emis_ref, skip_ref, gate_ref, up_ref, narrow_ref,
    gb_ref, coef_ref, norm_ref, taps_ref,
    out_ref,
    q_buf, k_buf, v_buf, valve_buf, cum_buf, pm_buf, h0_buf, run_buf, pair_buf, came_buf, went_buf, state_buf,
    att_buf, rows_buf, emis_buf, skip_buf, resid_buf, feats, gate_w, up_w, narrow_w, hidden,
    part_buf, half_buf, sum_buf, far_buf, out_buf,
    load_sem, own_sem, w_send, w_recv, pair_sem, chain_sem, att_send, att_recv, row_send, row_recv, halo_sem,
    half_send, half_recv, far_send, far_recv, out_sem,
):
    me, team_me = lax.axis_index("sp"), lax.axis_index("tp")
    spread, team = lax.axis_size("sp"), lax.axis_size("tp")
    ring, teams = spread // 2, team // 2
    place, side = me // 2, me % 2
    line, core = team_me // 2, team_me % 2
    length = v_buf.shape[1]
    chunks = length // CHUNK
    heads = v_buf.shape[0]
    width = feats.shape[1]
    share = length // team
    weights = (gate_w, up_w, narrow_w)
    block = gate_w.shape[0] // spread
    piece = block // 2
    started = []

    def go(wanted, make):
        if wanted is None:
            make().start()
        else:
            @pl.when(wanted)
            def _():
                make().start()

        started.append((wanted, make))

    def when(wanted, act):
        if wanted is None:
            act()
        else:
            pl.when(wanted)(act)

    loads = []

    def load(source, target):
        loads.append(pltpu.make_async_copy(source, target, load_sem.at[len(loads)]))
        loads[-1].start()

    own = []
    for which, ref in enumerate((gate_ref, up_ref, narrow_ref)):
        at = pl.ds(pl.multiple_of(me * block, block), block)
        own.append(pltpu.make_async_copy(ref, weights[which].at[at, :], own_sem.at[which]))
        own[-1].start()
    tiles = q_buf.shape[0]
    for tile in range(tiles):
        source = (q1_ref, k1_ref, tile) if tile < first else (q2_ref, k2_ref, tile - first)
        at = slice(source[2] * LANES, (source[2] + 1) * LANES)
        load(source[0].at[:, at], q_buf.at[tile])
        load(source[1].at[:, at], k_buf.at[tile])
    for head in range(heads):
        load(v_ref.at[:, head * LANES : (head + 1) * LANES], v_buf.at[head])
    early = len(loads)
    for head in range(heads):
        load(valve_ref.at[:, head * LANES : (head + 1) * LANES], valve_buf.at[head])
    middle = len(loads)
    load(skip_ref, skip_buf)
    load(emis_ref, emis_buf)

    barrier = pltpu.get_barrier_semaphore()
    for gap in (1, 2, spread - 2, spread - 1):
        pl.semaphore_signal(
            barrier, inc=1, device_id={"sp": lax.rem(me + gap, spread)}, device_id_type=MESH
        )
    for gap in range(1, team):
        pl.semaphore_signal(
            barrier, inc=1, device_id={"tp": lax.rem(team_me + gap, team)}, device_id_type=MESH
        )
    for one in own:
        one.wait()
    pl.semaphore_wait(barrier, 4 + team - 1)

    def block_copy(which, source, part, way):
        at = pl.ds(pl.multiple_of(source * block + part * piece, piece), piece)
        target = {UP: me + 2, DOWN: me - 2, ACROSS: me + 1 - 2 * side}[way]
        return pltpu.make_async_remote_copy(
            src_ref=weights[which].at[at, :],
            dst_ref=weights[which].at[at, :],
            send_sem=w_send.at[which, source, part, way],
            recv_sem=w_recv.at[which, source, part],
            device_id={"sp": target},
            device_id_type=MESH,
        )

    def send_line(which, part):
        go(place < ring - 1, lambda: block_copy(which, me, part, UP))
        go(place > 0, lambda: block_copy(which, me, part, DOWN))

    def send_across(which, part, rank):
        source = 2 * nearest(ring, place, rank) + side
        go(None, lambda: block_copy(which, source, part, ACROSS))

    def heard_across(which, part, rank):
        source = 2 * nearest(ring, place, rank) + 1 - side
        block_copy(which, source, part, ACROSS).wait_recv()

    def arrive(which, part, gap, held=None):
        low, high = me - 2 * gap, me + 2 * gap

        @pl.when(place >= gap)
        def _():
            block_copy(which, low, part, UP).wait_recv()

        @pl.when(place + gap < ring)
        def _():
            block_copy(which, high, part, DOWN).wait_recv()

        if gap < ring - 1:
            go((place + gap < ring) & (place > 0), lambda: block_copy(which, high, part, DOWN))
            onward = ((place >= gap) & (place < ring - 1), lambda: block_copy(which, low, part, UP))
            if held is None:
                go(*onward)
            else:
                held.append(onward)

    for which, part in ((0, 0), (0, 1), (1, 0)):
        send_across(which, part, 0)
        send_line(which, part)

    for chunk in range(chunks):
        at = slice(chunk * CHUNK, (chunk + 1) * CHUNK)
        level = gb_ref[:, at]
        cum = level
        lanes = lax.broadcasted_iota(jnp.int32, cum.shape, 1)
        shift = 1
        while shift < CHUNK:
            cum = cum + jnp.where(lanes >= shift, pltpu.roll(cum, shift, 1), 0.0)
            shift *= 2
        for head in range(heads):
            cum_buf[head, :, at] = cum[head : head + 1]
            cum_buf[heads + head, :, at] = level[heads + head : heads + head + 1]
    for one in loads[:early]:
        one.wait()

    def one_head(it, carry):
        attend_heads(
            first, it, q_buf, k_buf, v_buf, cum_buf, cum_buf, heads, pm_buf, h0_buf, run_buf,
            pair_buf.at[side],
        )
        return carry

    lax.fori_loop(0, heads, one_head, 0)

    def pair_copy():
        return pltpu.make_async_remote_copy(
            src_ref=pair_buf.at[side],
            dst_ref=pair_buf.at[side],
            send_sem=pair_sem.at[0],
            recv_sem=pair_sem.at[1],
            device_id={"sp": me + 1 - 2 * side},
            device_id_type=MESH,
        )

    go(None, pair_copy)
    send_across(1, 1, 0)
    send_line(1, 1)
    for one in loads[early:middle]:
        one.wait()
    pair_copy().wait_recv()
    held = []
    for part in range(2):
        arrive(0, part, 1, held)
        send_across(0, part, 1)

    def chain_copy():
        return pltpu.make_async_remote_copy(
            src_ref=went_buf,
            dst_ref=came_buf,
            send_sem=chain_sem.at[0],
            recv_sem=chain_sem.at[1],
            device_id={"sp": me + 2},
            device_id_type=MESH,
        )

    @pl.when(place == 0)
    def _():
        came_buf[...] = jnp.zeros_like(came_buf)

    @pl.when(place > 0)
    def _():
        chain_copy().wait_recv()

    before = [came_buf[head] for head in range(heads)]
    between = [
        mm(pair_buf[0, head, :, LANES:], before[head]) + pair_buf[0, head, :, :LANES].astype(F32)
        for head in range(heads)
    ]
    after = [
        mm(pair_buf[1, head, :, LANES:], between[head].astype(BF16))
        + pair_buf[1, head, :, :LANES].astype(F32)
        for head in range(heads)
    ]
    for head in range(heads):
        went_buf[head] = after[head].astype(BF16)
        state_buf[head] = jnp.where(side == 0, before[head].astype(F32), between[head]).astype(BF16)
    go(place < ring - 1, chain_copy)
    for onward in held:
        go(*onward)

    def finish(it, carry):
        coef = coef_ref[...]
        state = state_buf[it]
        starts = [
            (mm(run_buf[it, c, :, LANES:], state) + run_buf[it, c, :, :LANES].astype(F32)).astype(BF16)
            for c in range(chunks)
        ]
        lane = pl.ds(pl.multiple_of(it * LANES, LANES), LANES)
        for c in range(chunks):
            at = slice(c * CHUNK, (c + 1) * CHUNK)
            out = mm(pm_buf[it, at, :], starts[c]) + h0_buf[it, at, :]
            gate = valve_buf[it, at, :].astype(F32)
            scaled = out * lax.rsqrt(jnp.mean(out * out, axis=-1, keepdims=True) + EPSILON) * coef
            into, row = c * CHUNK // share, c * CHUNK % share
            att_buf[into, row : row + CHUNK, lane] = (
                scaled * (gate / (1.0 + jnp.exp(-gate)))
            ).astype(BF16)
        return carry

    lax.fori_loop(0, heads, finish, 0)

    mate = team_me + 1 - 2 * core
    others = []
    for gap in range(1, teams):
        there = lax.rem(line + gap, teams)
        others.append(2 * there + core)
        others.append(2 * there + 1 - core)

    def att_copy(source, target):
        return pltpu.make_async_remote_copy(
            src_ref=att_buf.at[target],
            dst_ref=rows_buf.at[source],
            send_sem=att_send.at[target],
            recv_sem=att_recv.at[source],
            device_id={"tp": target},
            device_id_type=MESH,
        )

    for peer in others + [mate]:
        go(None, functools.partial(att_copy, team_me, peer))
    for part in range(2):
        arrive(1, part, 1)
        send_across(1, part, 1)

    for one in loads[middle:]:
        one.wait()
    depth = rows_buf.shape[2] // 2

    def add_rows(x_ref, peer, start):
        for group in range(2):
            x = x_ref[:, group * depth : (group + 1) * depth]
            at = pl.ds(pl.multiple_of((group * team + peer) * depth, depth), depth)
            tile = min(512, width)
            for col in range(0, width, tile):
                base = (
                    skip_buf[:, col : col + tile].astype(F32)
                    if start and group == 0
                    else resid_buf[:, col : col + tile]
                )
                resid_buf[:, col : col + tile] = base + mm(x, emis_buf[at, col : col + tile])

    add_rows(att_buf.at[team_me], team_me, True)
    for peer in [mate] + others:
        att_copy(peer, team_me).wait_recv()
        add_rows(rows_buf.at[peer], peer, False)
    mine = pl.multiple_of(EDGE + team_me * share, EDGE)
    step = min(64, share)
    for row in range(0, share, step):
        total = resid_buf[row : row + step, :]
        scale = lax.rsqrt(jnp.mean(total * total, axis=-1, keepdims=True) + EPSILON)
        feats[pl.ds(mine + row, step), :] = (total * scale * norm_ref[...]).astype(BF16)

    row_part = share // 2

    def row_copy(source, target, part, slot):
        at = pl.ds(pl.multiple_of(EDGE + source * share + part * row_part, EDGE), row_part)
        return pltpu.make_async_remote_copy(
            src_ref=feats.at[at, :],
            dst_ref=feats.at[at, :],
            send_sem=row_send.at[slot, part],
            recv_sem=row_recv.at[source, part],
            device_id={"tp": target},
            device_id_type=MESH,
        )

    far = [2 * lax.rem(line + gap, teams) + core for gap in range(1, teams)]
    for part in range(2):
        for slot, peer in enumerate(far):
            go(None, functools.partial(row_copy, team_me, peer, part, 2 * slot + 1))
    for part in range(2):
        go(None, functools.partial(row_copy, team_me, mate, part, 0))
    for part in range(2):
        if ring > 2:
            arrive(0, part, 2)
            send_across(0, part, 2)
    for part in range(2):
        for slot, peer in enumerate(far):
            row_copy(peer, team_me, part, 0).wait_recv()
            go(None, functools.partial(row_copy, peer, mate, part, 2 * slot + 2))
    for part in range(2):
        row_copy(mate, team_me, part, 0).wait_recv()
        for peer in far:
            row_copy(peer + 1 - 2 * core, team_me, part, 0).wait_recv()

    def halo_copy():
        return pltpu.make_async_remote_copy(
            src_ref=feats.at[length:, :],
            dst_ref=feats.at[:EDGE, :],
            send_sem=halo_sem.at[0],
            recv_sem=halo_sem.at[1],
            device_id={"sp": me + 1},
            device_id_type=MESH,
        )

    go(me < spread - 1, halo_copy)

    @pl.when(me == 0)
    def _():
        feats[:EDGE, :] = jnp.zeros((EDGE, width), BF16)

    for part in range(2):
        if ring > 2:
            arrive(1, part, 2)
            send_across(1, part, 2)
    for part in range(2):
        send_line(2, part)
    for gap in range(3, ring):
        for which in range(2):
            for part in range(2):
                arrive(which, part, gap)
                send_across(which, part, gap)
    for part in range(2):
        send_across(2, part, 0)
    for part in range(2):
        arrive(2, part, 1)
        send_across(2, part, 1)
    for rank in range(ring):
        for which in range(2):
            for part in range(2):
                heard_across(which, part, rank)

    @pl.when(me > 0)
    def _():
        halo_copy().wait_recv()

    units = hidden.shape[1]
    wide = min(256, units)
    tall = min(512, length)
    turns = units // wide * (length // tall)

    def hidden_tile(turn, carry):
        col = pl.ds(pl.multiple_of(turn // (length // tall) * wide, wide), wide)
        row = pl.multiple_of(turn % (length // tall) * tall, tall)
        x = feats[pl.ds(row, tall + EDGE), :]
        taken = []
        for which in range(2):
            low = mm(x, weights[which][:, col]).astype(BF16).astype(F32)
            total = 0.0
            for tap in range(TAPS):
                moved = low[EDGE - TAPS + 1 + tap : EDGE - TAPS + 1 + tap + tall]
                total = total + taps_ref[2 * tap + which : 2 * tap + which + 1, col] * moved
            taken.append(total)
        gate, up = taken
        hidden[pl.ds(row, tall), col] = (gate / (1.0 + jnp.exp(-gate)) * up).astype(BF16)
        return carry

    cuts = [turns * cut // (ring - 1) for cut in range(ring)]
    for cut in range(ring - 1):
        lax.fori_loop(cuts[cut], cuts[cut + 1], hidden_tile, 0)
        gap = cut + 2
        if gap < ring:
            for part in range(2):
                arrive(2, part, gap)
                send_across(2, part, gap)

    def owner(turn):
        rank = nearest(ring, place, turn % ring)
        return 2 * rank + (side if turn < ring else 1 - side)

    def half_copy(turn, there):
        at = pl.ds(pl.multiple_of((2 * there + 1 - core) * share, share), share)
        return pltpu.make_async_remote_copy(
            src_ref=part_buf.at[turn, at, :],
            dst_ref=half_buf.at[turn, there],
            send_sem=half_send.at[turn, there],
            recv_sem=half_recv.at[turn, there],
            device_id={"tp": mate},
            device_id_type=MESH,
        )

    def far_copy(turn, there, source):
        return pltpu.make_async_remote_copy(
            src_ref=sum_buf.at[turn, there],
            dst_ref=far_buf.at[turn, source],
            send_sem=far_send.at[turn, there],
            recv_sem=far_recv.at[turn, source],
            device_id={"tp": 2 * there + core},
            device_id_type=MESH,
        )

    def both(turn, there):
        at = pl.ds(pl.multiple_of((2 * there + core) * share, share), share)
        return part_buf[turn, at, :].astype(F32) + half_buf[turn, there].astype(F32)

    def product(turn):
        source = owner(turn)
        if turn >= ring:
            for part in range(2):
                heard_across(2, part, turn % ring)
        at = pl.ds(pl.multiple_of(source * block, block), block)
        part_buf[turn] = mm_nt(hidden[...], narrow_w[at, :]).astype(BF16)
        for there in range(teams):
            go(None, functools.partial(half_copy, turn, there))

    def pass_on(turn):
        for there in range(teams):
            half_copy(turn, there).wait_recv()
        for gap in range(1, teams):
            there = lax.rem(line + gap, teams)
            sum_buf[turn, there] = both(turn, there).astype(BF16)
            go(None, functools.partial(far_copy, turn, there, line))

    def close(turn):
        col = pl.ds(pl.multiple_of(owner(turn) * block, block), block)
        total = resid_buf[:, col] + both(turn, line)
        for gap in range(1, teams):
            there = lax.rem(line + gap, teams)
            far_copy(turn, line, there).wait_recv()
            total = total + far_buf[turn, there].astype(F32)
        out_buf[:, col] = total.astype(BF16)
        put(turn).start()

    def put(turn):
        col = pl.ds(pl.multiple_of(owner(turn) * block, block), block)
        return pltpu.make_async_copy(out_buf.at[:, col], out_ref.at[:, col], out_sem.at[turn])

    for turn in range(spread + 2):
        if turn < spread:
            product(turn)
        if 1 <= turn <= spread:
            pass_on(turn - 1)
        if turn >= 2:
            close(turn - 2)
    for turn in range(spread):
        put(turn).wait()
    for wanted, make in started:
        when(wanted, lambda make=make: make().wait_send())


def whole_step(first, q1, k1, q2, k2, v, valve, emis, skip, gate, up, narrow, gb, coef, norm, taps):
    spread, team = lax.axis_size("sp"), lax.axis_size("tp")
    teams = team // 2
    length = q1.shape[0]
    heads = v.shape[1] // LANES
    chunks = length // CHUNK
    tiles = (q1.shape[1] + q2.shape[1]) // LANES
    share, width = skip.shape
    block, units = gate.shape
    anywhere = pl.BlockSpec(memory_space=pl.ANY)
    inside = pl.BlockSpec(memory_space=pltpu.VMEM)
    dma = pltpu.SemaphoreType.DMA

    def vmem(*shape, dtype=BF16):
        return pltpu.VMEM(shape, dtype)

    scratch = [
        vmem(tiles, length, LANES),
        vmem(tiles, length, LANES),
        vmem(heads, length, LANES),
        vmem(heads, length, LANES),
        vmem(2 * heads, 1, length, dtype=F32),
        vmem(heads, length, LANES),
        vmem(heads, length, LANES, dtype=F32),
        vmem(heads, chunks, LANES, 2 * LANES),
        vmem(2, heads, LANES, 2 * LANES),
        vmem(heads, LANES, LANES),
        vmem(heads, LANES, LANES),
        vmem(heads, LANES, LANES),
        vmem(team, share, heads * LANES),
        vmem(team, share, heads * LANES),
        vmem(*emis.shape),
        vmem(share, width),
        vmem(share, width, dtype=F32),
        vmem(EDGE + length, width),
        vmem(width, units),
        vmem(width, units),
        vmem(width, units),
        vmem(length, units),
        vmem(spread, length, block),
        vmem(spread, teams, share, block),
        vmem(spread, teams, share, block),
        vmem(spread, teams, share, block),
        vmem(share, width),
        dma((2 * tiles + 2 * heads + 2,)),
        dma((3,)),
        dma((3, spread, 2, 3)),
        dma((3, spread, 2)),
        dma((2,)),
        dma((2,)),
        dma((team,)),
        dma((team,)),
        dma((2 * teams, 2)),
        dma((team, 2)),
        dma((2,)),
        dma((spread, teams)),
        dma((spread, teams)),
        dma((spread, teams)),
        dma((spread, teams)),
        dma((spread,)),
    ]
    return pl.pallas_call(
        functools.partial(step_kernel, first),
        in_specs=[anywhere] * 11 + [inside] * 4,
        out_specs=anywhere,
        out_shape=jax.ShapeDtypeStruct((share, width), BF16),
        scratch_shapes=scratch,
        compiler_params=pltpu.CompilerParams(
            collective_id=1, has_side_effects=True, vmem_limit_bytes=67043328
        ),
        cost_estimate=pl.CostEstimate(flops=10**11, bytes_accessed=10**8, transcendentals=0),
    )(q1, k1, q2, k2, v, valve, emis, skip, gate, up, narrow, gb, coef, norm, taps)


def per_device(
    arriving_hidden_state,
    former_request_vectors,
    former_match_vectors,
    latter_request_vectors,
    latter_match_vectors,
    stored_vectors_both,
    closing_valve_operands,
    update_level_before_squash,
    fading_data_input,
    sparse_fading_boost,
    unitwise_fading_loglevel,
    fading_constant_term,
    unitwise_normalizer_coef,
    emission_map_weights,
    channel_normalizer_coef,
    switching_channel_map,
    broadening_channel_map,
    timewise_convolve_tapvalues,
    narrowing_map_weights_in,
):
    length = former_request_vectors.shape[0]
    level = (
        -jnp.exp(unitwise_fading_loglevel)[..., None]
        * jax.nn.softplus(fading_data_input + fading_constant_term[..., None])
        + sparse_fading_boost
    )
    beta_rate = jax.nn.sigmoid(update_level_before_squash.astype(jnp.float32))
    gates_beta = jnp.concatenate([level, beta_rate], axis=0).reshape(-1, length)
    gates_beta = jnp.pad(gates_beta, ((0, -gates_beta.shape[0] % 8), (0, 0)))
    spare = -latter_request_vectors.shape[1] % LANES
    return whole_step(
        former_request_vectors.shape[1] // LANES,
        former_request_vectors,
        former_match_vectors,
        jnp.pad(latter_request_vectors, ((0, 0), (0, spare))),
        jnp.pad(latter_match_vectors, ((0, 0), (0, spare))),
        stored_vectors_both.reshape(length, -1),
        closing_valve_operands.reshape(length, -1),
        emission_map_weights,
        arriving_hidden_state,
        switching_channel_map,
        broadening_channel_map,
        narrowing_map_weights_in,
        gates_beta,
        unitwise_normalizer_coef.reshape(1, -1),
        channel_normalizer_coef.reshape(1, -1),
        timewise_convolve_tapvalues.astype(F32).reshape(2 * TAPS, -1),
    )


def solution(mesh):
    placed = (
        P(("sp", "tp"), None),
        P("sp", "tp"),
        P("sp", "tp"),
        P("sp", "tp"),
        P("sp", "tp"),
        P("sp", None, "tp"),
        P("sp", None, "tp"),
        P(None, "tp", "sp"),
        P(None, "tp", "sp"),
        P(None, "tp", "sp"),
        P(None, "tp"),
        P(None, "tp"),
        P(),
        P(),
        P(),
        P("sp", "tp"),
        P("sp", "tp"),
        P(None, None, "tp"),
        P("sp", "tp"),
    )
    return jax.shard_map(
        per_device, mesh=mesh, in_specs=placed, out_specs=P(("sp", "tp"), None), check_vma=False
    )
```

```python
import functools

import jax
import jax.numpy as jnp
from jax import lax
from jax.experimental import pallas as pl
from jax.experimental.pallas import tpu as pltpu
from jax.sharding import PartitionSpec as P

TAPS = 3
CHUNK = 128
BASE = 16
LANES = 128
EDGE = 16
UP, DOWN, ACROSS = 0, 1, 2

EPSILON = 1e-06
F32 = jnp.float32
BF16 = jnp.bfloat16
MESH = pl.DeviceIdType.MESH


def mm(a, b):
    return jnp.dot(a, b, preferred_element_type=F32)


def mm_nt(a, b):
    return lax.dot_general(a, b, (((1,), (1,)), ((), ())), preferred_element_type=F32)


def attend_heads(first, it, q_ref, k_ref, v_ref, cum_ref, gb_ref, heads, pm_ref, h0_ref, run_ref, last_ref):
    n = v_ref.shape[1] // CHUNK
    rows = lax.broadcasted_iota(jnp.int32, (CHUNK, CHUNK), 0)
    cols = lax.broadcasted_iota(jnp.int32, (CHUNK, CHUNK), 1)
    causal = rows >= cols
    eye = (rows == cols).astype(F32)
    lane = lax.broadcasted_iota(jnp.int32, (1, LANES), 1)
    narrow = it >= first
    other = jnp.maximum(it - first, 0)
    tile = jnp.where(narrow, first + other // 2, it)
    own = (lane // (LANES // 2) == other % 2) | jnp.logical_not(narrow)
    keep = jnp.where(own, 1.0, 0.0)
    diag = jnp.where(own, eye, 0.0)
    scale = jnp.where(narrow, (LANES // 2) ** -0.5, LANES ** -0.5)
    R = range(n)
    at = [pl.ds(c * CHUNK, CHUNK) for c in R]
    ks, qs, vs, low, intra, grown, fall, total, betas = ([None] * n for _ in range(9))
    for c in R:
        q = q_ref[tile, at[c], :].astype(F32) * keep
        k = k_ref[tile, at[c], :].astype(F32) * keep
        q = q * (lax.rsqrt(jnp.sum(q * q, axis=-1, keepdims=True) + EPSILON) * scale)
        k = k * lax.rsqrt(jnp.sum(k * k, axis=-1, keepdims=True) + EPSILON)
        cum = cum_ref[it, :, at[c]]
        beta = cum_ref[heads + it, :, at[c]]
        crow = jnp.broadcast_to(cum, (CHUNK, CHUNK))
        ccol = crow.T
        bcol = jnp.broadcast_to(beta, (CHUNK, CHUNK)).T
        total[c] = crow[:, CHUNK - 1:]
        decay = jnp.exp(jnp.where(causal, ccol - crow, -1e30))
        grown[c] = jnp.exp(ccol)
        kb = k.astype(BF16)
        kbeta = k * bcol
        both = mm_nt(jnp.concatenate([kbeta.astype(BF16), q.astype(BF16)], axis=0), kb)
        low[c] = jnp.where(rows > cols, both[:CHUNK] * decay, 0.0)
        intra[c] = (both[CHUNK:] * decay).astype(BF16)
        fall[c] = (k.T * jnp.exp(crow[:, CHUNK-1:] - crow)).astype(BF16)
        ks[c] = (kbeta * grown[c]).astype(BF16)
        vs[c] = (v_ref[it, at[c], :].astype(F32) * bcol).astype(BF16)
        qs[c] = q * grown[c]
    inner = (rows // BASE) == (cols // BASE)
    power = [jnp.where(inner, low[c], 0.0) for c in R]
    inv = [eye - power[c] for c in R]
    power = [p.astype(BF16) for p in power]
    size = 2
    while size < BASE:
        power = [mm(p, p).astype(BF16) for p in power]
        inv = [i + mm(i.astype(BF16), p) for i, p in zip(inv, power)]
        size *= 2
    block = BASE
    while block < CHUNK:
        here = ((rows // (2 * block)) == (cols // (2 * block))) & ((rows // block) != (cols // block))
        invb = [i.astype(BF16) for i in inv]
        half = [mm(invb[c], jnp.where(here, low[c], 0.0).astype(BF16)).astype(BF16) for c in R]
        inv = [inv[c] - mm(half[c], invb[c]) for c in R]
        block *= 2
    solved = [mm(inv[c].astype(BF16), jnp.concatenate([vs[c], ks[c]], axis=-1)).astype(BF16) for c in R]
    out = [mm(jnp.concatenate([fall[c], intra[c]], axis=0), solved[c]) for c in R]
    for c in R:
        h0_ref[it, at[c], :] = out[c][CHUNK:, :LANES]
        pm_ref[it, at[c], :] = (qs[c] - out[c][CHUNK:, LANES:]).astype(BF16)
    run = jnp.concatenate([jnp.zeros((LANES, LANES), F32), diag], axis=-1)
    for c in R:
        run_ref[it, c] = run.astype(BF16)
        cmap = (jnp.exp(total[c]) * diag - out[c][:CHUNK, LANES:]).astype(BF16)
        nxt = mm(cmap, run.astype(BF16))
        run = jnp.concatenate([nxt[:, :LANES] + out[c][:CHUNK, :LANES], nxt[:, LANES:]], axis=-1)
    last_ref[it] = run.astype(BF16)


def nearest(ring, place, rank):
    found = 0
    for here in range(ring):
        table = sorted(range(ring), key=lambda other: (abs(other - here), other))
        found = found + jnp.where(place == here, table[rank], 0)
    return found


def step_kernel(
    first,
    q1_ref, k1_ref, q2_ref, k2_ref, v_ref, valve_ref, emis_ref, skip_ref, gate_ref, up_ref, narrow_ref,
    gb_ref, coef_ref, norm_ref, taps_ref,
    out_ref,
    q_buf, k_buf, v_buf, valve_buf, v_raw, valve_raw, cum_buf, pm_buf, h0_buf, run_buf, pair_buf, came_buf, went_buf, state_buf,
    att_buf, rows_buf, emis_buf, skip_buf, resid_buf, feats, gate_w, up_w, narrow_w, hidden,
    half_buf, far_buf, out_buf,
    load_sem, own_sem, w_send, w_recv, pair_sem, chain_sem, att_send, att_recv, row_send, row_recv, halo_sem,
    half_send, half_recv, far_send, far_recv, out_sem,
):
    me, team_me = lax.axis_index("sp"), lax.axis_index("tp")
    spread, team = lax.axis_size("sp"), lax.axis_size("tp")
    ring, teams = spread // 2, team // 2
    place, side = me // 2, me % 2
    line, core = team_me // 2, team_me % 2
    length = v_buf.shape[1]
    chunks = length // CHUNK
    heads = v_buf.shape[0]
    width = feats.shape[1]
    share = length // team
    weights = (gate_w, up_w, narrow_w)
    block = gate_w.shape[0] // spread
    units = gate_w.shape[1]
    partner = me + 1 - 2 * side
    started = []

    def go(wanted, make):
        if wanted is None:
            make().start()
        else:
            @pl.when(wanted)
            def _():
                make().start()

        started.append((wanted, make))

    def when(wanted, act):
        if wanted is None:
            act()
        else:
            pl.when(wanted)(act)

    loads = []

    def load(source, target):
        loads.append(pltpu.make_async_copy(source, target, load_sem.at[len(loads)]))
        loads[-1].start()

    own = []
    for which, ref in enumerate((gate_ref, up_ref, narrow_ref)):
        at = pl.ds(pl.multiple_of(me * block, block), block)
        col = pl.ds(pl.multiple_of(side * units, LANES), units)
        own.append(pltpu.make_async_copy(ref.at[:, col], weights[which].at[at, :], own_sem.at[which]))
        own[-1].start()
    tiles = q_buf.shape[0]
    for tile in range(tiles):
        source = (q1_ref, k1_ref, tile) if tile < first else (q2_ref, k2_ref, tile - first)
        at = slice(source[2] * LANES, (source[2] + 1) * LANES)
        load(source[0].at[:, at], q_buf.at[tile])
        load(source[1].at[:, at], k_buf.at[tile])
    load(v_ref, v_raw)
    early = len(loads)
    load(valve_ref, valve_raw)
    middle = len(loads)

    def by_head(raw, into):
        def turn(c, carry):
            at = pl.ds(pl.multiple_of(c * CHUNK, CHUNK), CHUNK)
            rows = raw[at, :, :].astype(F32)
            for head in range(heads):
                group, here = head // (heads // 2), head % (heads // 2)
                into[head, at, :] = rows[:, group, here * LANES : (here + 1) * LANES].astype(BF16)
            return carry

        lax.fori_loop(0, chunks, turn, 0)
    load(skip_ref, skip_buf)
    load(emis_ref, emis_buf)

    barrier = pltpu.get_barrier_semaphore()
    for gap in (2, spread - 2):
        pl.semaphore_signal(
            barrier, inc=1, device_id={"sp": lax.rem(me + gap, spread)}, device_id_type=MESH
        )
    for there in range(teams):
        pl.semaphore_signal(
            barrier,
            inc=1,
            device_id={"sp": partner, "tp": 2 * there + core},
            device_id_type=MESH,
        )
    for gap in range(1, team):
        pl.semaphore_signal(
            barrier, inc=1, device_id={"tp": lax.rem(team_me + gap, team)}, device_id_type=MESH
        )
    for one in own:
        one.wait()
    pl.semaphore_wait(barrier, 2 + teams + team - 1)

    def owner(there, part):
        return 2 * there + (side if part == 0 else 1 - side)

    def block_copy(which, there, part, way):
        source = owner(there, part)
        at = pl.ds(pl.multiple_of(source * block, block), block)
        return pltpu.make_async_remote_copy(
            src_ref=weights[which].at[at, :],
            dst_ref=weights[which].at[at, :],
            send_sem=w_send.at[which, source, way],
            recv_sem=w_recv.at[which, source],
            device_id={"sp": me + 2 if way == UP else me - 2},
            device_id_type=MESH,
        )

    def across_copy(which, source):
        at = pl.ds(pl.multiple_of(source * block, block), block)
        col = pl.ds(pl.multiple_of((1 - side) * units, LANES), units)
        return pltpu.make_async_remote_copy(
            src_ref=(gate_ref, up_ref, narrow_ref)[which].at[:, col],
            dst_ref=weights[which].at[at, :],
            send_sem=w_send.at[which, source, ACROSS],
            recv_sem=w_recv.at[which, source],
            device_id={"sp": partner},
            device_id_type=MESH,
        )

    def send_across(which):
        go(None, lambda: across_copy(which, me))

    def send_line(which, part):
        if part:
            across_copy(which, partner).wait_recv()
        go(place < ring - 1, lambda: block_copy(which, place, part, UP))
        go(place > 0, lambda: block_copy(which, place, part, DOWN))

    def arrive(which, part, gap, held=None):
        low, high = place - gap, place + gap

        @pl.when(place >= gap)
        def _():
            block_copy(which, low, part, UP).wait_recv()

        @pl.when(place + gap < ring)
        def _():
            block_copy(which, high, part, DOWN).wait_recv()

        if gap < ring - 1:
            go((place + gap < ring) & (place > 0), lambda: block_copy(which, high, part, DOWN))
            wanted = (place >= gap) & (place < ring - 1)
            make = lambda: block_copy(which, low, part, UP)
            if held is None:
                go(wanted, make)
            else:
                go(wanted & (place == ring - 2), make)
                held.append((wanted & (place < ring - 2), make))

    for which in range(2):
        send_across(which)
        send_line(which, 0)
    send_line(2, 0)

    for chunk in range(chunks):
        at = slice(chunk * CHUNK, (chunk + 1) * CHUNK)
        level = gb_ref[:, at]
        cum = level
        lanes = lax.broadcasted_iota(jnp.int32, cum.shape, 1)
        shift = 1
        while shift < CHUNK:
            cum = cum + jnp.where(lanes >= shift, pltpu.roll(cum, shift, 1), 0.0)
            shift *= 2
        for head in range(heads):
            cum_buf[head, :, at] = cum[head : head + 1]
            cum_buf[heads + head, :, at] = level[heads + head : heads + head + 1]
    for one in loads[:early]:
        one.wait()
    by_head(v_raw, v_buf)

    def one_head(it, carry):
        attend_heads(
            first, it, q_buf, k_buf, v_buf, cum_buf, cum_buf, heads, pm_buf, h0_buf, run_buf,
            pair_buf.at[side],
        )
        return carry

    lax.fori_loop(0, heads, one_head, 0)

    def pair_copy():
        return pltpu.make_async_remote_copy(
            src_ref=pair_buf.at[side],
            dst_ref=pair_buf.at[side],
            send_sem=pair_sem.at[0],
            recv_sem=pair_sem.at[1],
            device_id={"sp": partner},
            device_id_type=MESH,
        )

    go(None, pair_copy)
    send_across(2)
    for which in range(2):
        send_line(which, 1)
    held = []
    if ring > 1:
        arrive(0, 0, 1, held)
    for one in loads[early:middle]:
        one.wait()
    by_head(valve_raw, valve_buf)
    pair_copy().wait_recv()

    def chain_copy():
        return pltpu.make_async_remote_copy(
            src_ref=went_buf,
            dst_ref=came_buf,
            send_sem=chain_sem.at[0],
            recv_sem=chain_sem.at[1],
            device_id={"sp": me + 2},
            device_id_type=MESH,
        )

    @pl.when(place == 0)
    def _():
        came_buf[...] = jnp.zeros_like(came_buf)

    @pl.when(place > 0)
    def _():
        chain_copy().wait_recv()

    before = [came_buf[head] for head in range(heads)]
    between = [
        mm(pair_buf[0, head, :, LANES:], before[head]) + pair_buf[0, head, :, :LANES].astype(F32)
        for head in range(heads)
    ]
    after = [
        mm(pair_buf[1, head, :, LANES:], between[head].astype(BF16))
        + pair_buf[1, head, :, :LANES].astype(F32)
        for head in range(heads)
    ]
    for head in range(heads):
        went_buf[head] = after[head].astype(BF16)
        state_buf[head] = jnp.where(side == 0, before[head].astype(F32), between[head]).astype(BF16)
    go(place < ring - 1, chain_copy)
    for onward in held:
        go(*onward)
    arrive(1, 0, 1)

    def finish(it, carry):
        coef = coef_ref[...]
        state = state_buf[it]
        starts = [
            (mm(run_buf[it, c, :, LANES:], state) + run_buf[it, c, :, :LANES].astype(F32)).astype(BF16)
            for c in range(chunks)
        ]
        lane = pl.ds(pl.multiple_of(it * LANES, LANES), LANES)
        for c in range(chunks):
            at = slice(c * CHUNK, (c + 1) * CHUNK)
            out = mm(pm_buf[it, at, :], starts[c]) + h0_buf[it, at, :]
            gate = valve_buf[it, at, :].astype(F32)
            scaled = out * lax.rsqrt(jnp.mean(out * out, axis=-1, keepdims=True) + EPSILON) * coef
            into, row = c * CHUNK // share, c * CHUNK % share
            att_buf[into, row : row + CHUNK, lane] = (
                scaled * (gate / (1.0 + jnp.exp(-gate)))
            ).astype(BF16)
        return carry

    lax.fori_loop(0, heads, finish, 0)

    mate = team_me + 1 - 2 * core
    others = []
    for gap in range(1, teams):
        there = lax.rem(line + gap, teams)
        others.append(2 * there + core)
        others.append(2 * there + 1 - core)

    def att_copy(source, target):
        return pltpu.make_async_remote_copy(
            src_ref=att_buf.at[target],
            dst_ref=rows_buf.at[source],
            send_sem=att_send.at[target],
            recv_sem=att_recv.at[source],
            device_id={"tp": target},
            device_id_type=MESH,
        )

    for peer in others + [mate]:
        go(None, functools.partial(att_copy, team_me, peer))
    arrive(0, 1, 1)
    arrive(1, 1, 1)
    for which in range(2):
        if ring > 2:
            arrive(which, 0, 2)

    for one in loads[middle:]:
        one.wait()
    depth = rows_buf.shape[2] // 2

    def add_rows(x_ref, peer, start):
        for group in range(2):
            x = x_ref[:, group * depth : (group + 1) * depth]
            at = pl.ds(pl.multiple_of((group * team + peer) * depth, depth), depth)
            tile = min(512, width)
            for col in range(0, width, tile):
                base = (
                    skip_buf[:, col : col + tile].astype(F32)
                    if start and group == 0
                    else resid_buf[:, col : col + tile]
                )
                resid_buf[:, col : col + tile] = base + mm(x, emis_buf[at, col : col + tile])

    add_rows(att_buf.at[team_me], team_me, True)
    for peer in [mate] + others:
        att_copy(peer, team_me).wait_recv()
        add_rows(rows_buf.at[peer], peer, False)
    here = side * team + team_me
    mine = pl.multiple_of(EDGE + here * share, EDGE)
    step = min(64, share)
    for row in range(0, share, step):
        total = resid_buf[row : row + step, :]
        scale = lax.rsqrt(jnp.mean(total * total, axis=-1, keepdims=True) + EPSILON)
        feats[pl.ds(mine + row, step), :] = (total * scale * norm_ref[...]).astype(BF16)

    row_part = share // 2

    def row_copy(source, part, way, target):
        at = pl.ds(pl.multiple_of(EDGE + source * share + part * row_part, EDGE), row_part)
        return pltpu.make_async_remote_copy(
            src_ref=feats.at[at, :],
            dst_ref=feats.at[at, :],
            send_sem=row_send.at[source, part, way],
            recv_sem=row_recv.at[source, part],
            device_id=target,
            device_id_type=MESH,
        )

    def row_index(group, there, lane):
        return group * team + 2 * there + lane

    def row_arrive(source, part):
        row_copy(source, part, 0, {"tp": mate}).wait_recv()

    def row_send_to(source, part, way, target):
        go(None, lambda: row_copy(source, part, way, target))

    aside = [lax.rem(line + gap, teams) for gap in range(1, teams)]
    for part in range(2):
        for gap, there in enumerate(aside):
            row_send_to(here, part, 2 + gap, {"tp": 2 * there + core})
        row_send_to(here, part, 1, {"sp": partner})
    for part in range(2):
        row_send_to(here, part, 0, {"tp": mate})
    for which in range(2):
        if ring > 2:
            arrive(which, 1, 2)
    send_line(2, 1)
    beyond = row_index(1 - side, line, core)
    row_arrive(beyond, 0)
    for gap, there in enumerate(aside):
        row_send_to(beyond, 0, 2 + gap, {"tp": 2 * there + core})
    row_send_to(beyond, 0, 0, {"tp": mate})
    for there in aside:
        row_arrive(row_index(side, there, core), 0)
        row_send_to(row_index(side, there, core), 0, 0, {"tp": mate})
    for there in aside:
        row_arrive(row_index(side, there, core), 1)
        row_send_to(row_index(side, there, core), 1, 1, {"sp": partner})
        row_send_to(row_index(side, there, core), 1, 0, {"tp": mate})
    row_arrive(beyond, 1)
    row_send_to(beyond, 1, 0, {"tp": mate})
    for there in aside:
        for part in range(2):
            row_arrive(row_index(1 - side, there, core), part)
            row_send_to(row_index(1 - side, there, core), part, 0, {"tp": mate})
    for part in range(2):
        for group in range(2):
            for there in range(teams):
                row_arrive(row_index(group, there, 1 - core), part)

    def halo_copy():
        return pltpu.make_async_remote_copy(
            src_ref=feats.at[2 * length :, :],
            dst_ref=feats.at[:EDGE, :],
            send_sem=halo_sem.at[0],
            recv_sem=halo_sem.at[1],
            device_id={"sp": me + 2},
            device_id_type=MESH,
        )

    go(place < ring - 1, halo_copy)

    @pl.when(place == 0)
    def _():
        feats[:EDGE, :] = jnp.zeros((EDGE, width), BF16)

    for gap in range(3, ring):
        for part in range(2):
            for which in range(2):
                arrive(which, part, gap)
    arrive(2, 0, 1)

    @pl.when(place > 0)
    def _():
        halo_copy().wait_recv()

    wide = 256 if units % 256 == 0 else LANES
    tall = 2 * share

    def hidden_rows(row):
        def tile(turn, carry):
            col = pl.ds(pl.multiple_of(turn * wide, wide), wide)
            tap_col = pl.ds(pl.multiple_of(side * units + turn * wide, LANES), wide)
            x = feats[pl.ds(row, tall + EDGE), :]
            taken = []
            for which in range(2):
                low = mm(x, weights[which][:, col]).astype(BF16).astype(F32)
                total = 0.0
                for tap in range(TAPS):
                    moved = low[EDGE - TAPS + 1 + tap : EDGE - TAPS + 1 + tap + tall]
                    total = total + taps_ref[2 * tap + which : 2 * tap + which + 1, tap_col] * moved
                taken.append(total)
            gate, up = taken
            hidden[pl.ds(row, tall), col] = (gate / (1.0 + jnp.exp(-gate)) * up).astype(BF16)
            return carry

        lax.fori_loop(0, units // wide, tile, 0)

    part_buf = emis_buf
    early_turns = range(min(3, spread))
    seen = {(0, 1)}
    chips = [(ds, dl) for ds in range(2) for dl in range(teams)]

    def chip(ds, dl):
        return (side + ds) % 2, lax.rem(line + dl, teams)

    def chip_at(ds, dl):
        group, there = chip(ds, dl)
        return group * teams + there

    def rows_of(ds, dl, lane):
        group, there = chip(ds, dl)
        return pl.ds(pl.multiple_of(row_index(group, there, lane) * share, share), share)

    def half_copy(turn, ds, dl):
        return pltpu.make_async_remote_copy(
            src_ref=part_buf.at[rows_of(ds, dl, 1 - core), turn * block : (turn + 1) * block],
            dst_ref=half_buf.at[turn, chip_at(ds, dl)],
            send_sem=half_send.at[turn, chip_at(ds, dl)],
            recv_sem=half_recv.at[turn, chip_at(ds, dl)],
            device_id={"tp": mate},
            device_id_type=MESH,
        )

    def far_copy(turn, ds, dl, heard):
        group, there = chip(ds, dl)
        slot = chip_at(ds, dl) if heard else chip_at(0, 0)
        target = turn if heard or ds == 0 else turn + 1 - 2 * (turn % 2)
        return pltpu.make_async_remote_copy(
            src_ref=half_buf.at[turn, chip_at(ds, dl)],
            dst_ref=far_buf.at[target, slot],
            send_sem=far_send.at[turn, chip_at(ds, dl)],
            recv_sem=far_recv.at[target, slot],
            device_id={"sp": 2 * place + group, "tp": 2 * there + core},
            device_id_type=MESH,
        )

    def both(turn, ds, dl):
        mine = part_buf[rows_of(ds, dl, core), turn * block : (turn + 1) * block]
        return mine.astype(F32) + half_buf[turn, chip_at(ds, dl)].astype(F32)

    def source_of(turn):
        return owner(nearest(ring, place, turn // 2), turn % 2)

    def hear(part, gap):
        if 0 < gap < ring and (part, gap) not in seen:
            seen.add((part, gap))
            arrive(2, part, gap)

    def product(turn, ds, dl):
        at = pl.ds(pl.multiple_of(source_of(turn) * block, block), block)
        row = pl.ds(pl.multiple_of(chip_at(ds, dl) * tall, tall), tall)
        part_buf[row, turn * block : (turn + 1) * block] = mm_nt(
            hidden[row, :], narrow_w[at, :]
        ).astype(BF16)
        go(None, functools.partial(half_copy, turn, ds, dl))

    def pass_on(turn, ds, dl):
        half_copy(turn, ds, dl).wait_recv()
        if (ds, dl) != (0, 0):
            half_buf[turn, chip_at(ds, dl)] = both(turn, ds, dl).astype(BF16)
            go(None, functools.partial(far_copy, turn, ds, dl, False))

    def close(turn):
        col = pl.ds(pl.multiple_of(source_of(turn) * block, block), block)
        total = resid_buf[:, col] + both(turn, 0, 0)
        for ds, dl in chips[1:]:
            far_copy(turn, ds, dl, True).wait_recv()
            total = total + far_buf[turn, chip_at(ds, dl)].astype(F32)
        out_buf[:, col] = total.astype(BF16)
        put(turn).start()

    def put(turn):
        col = pl.ds(pl.multiple_of(source_of(turn) * block, block), block)
        return pltpu.make_async_copy(out_buf.at[:, col], out_ref.at[:, col], out_sem.at[turn])

    farthest = sorted(chips, key=lambda c: (-(c[0] + (c[1] > 0)), c))
    waiting = []
    for count, (ds, dl) in enumerate(farthest):
        hidden_rows(pl.multiple_of(chip_at(ds, dl) * tall, tall))
        for one in waiting:
            pass_on(*one)
        waiting = [(turn, ds, dl) for turn in early_turns]
        for one in waiting:
            product(*one)
        if count == 1:
            hear(1, 1)
        if count == len(chips) - 1:
            hear(0, 2)
    open_turns = list(early_turns)
    for turn in range(len(early_turns), spread):
        hear(turn % 2, turn // 2)
        for ds, dl in farthest:
            product(turn, ds, dl)
        for one in waiting:
            pass_on(*one)
        waiting = [(turn, ds, dl) for ds, dl in farthest]
        close(open_turns.pop(0))
        open_turns.append(turn)
    for one in waiting:
        pass_on(*one)
    for turn in open_turns:
        close(turn)
    for turn in range(spread):
        put(turn).wait()
    for wanted, make in started:
        when(wanted, lambda make=make: make().wait_send())


def whole_step(first, q1, k1, q2, k2, v, valve, emis, skip, gate, up, narrow, gb, coef, norm, taps):
    spread, team = lax.axis_size("sp"), lax.axis_size("tp")
    teams = team // 2
    length = q1.shape[0]
    heads = 2 * v.shape[2] // LANES
    chunks = length // CHUNK
    tiles = (q1.shape[1] + q2.shape[1]) // LANES
    share, width = skip.shape
    block, units = gate.shape[0], gate.shape[1] // 2
    anywhere = pl.BlockSpec(memory_space=pl.ANY)
    inside = pl.BlockSpec(memory_space=pltpu.VMEM)
    dma = pltpu.SemaphoreType.DMA

    def vmem(*shape, dtype=BF16):
        return pltpu.VMEM(shape, dtype)

    scratch = [
        vmem(tiles, length, LANES),
        vmem(tiles, length, LANES),
        vmem(heads, length, LANES),
        vmem(heads, length, LANES),
        vmem(*v.shape),
        vmem(*v.shape),
        vmem(2 * heads, 1, length, dtype=F32),
        vmem(heads, length, LANES),
        vmem(heads, length, LANES, dtype=F32),
        vmem(heads, chunks, LANES, 2 * LANES),
        vmem(2, heads, LANES, 2 * LANES),
        vmem(heads, LANES, LANES),
        vmem(heads, LANES, LANES),
        vmem(heads, LANES, LANES),
        vmem(team, share, heads * LANES),
        vmem(team, share, heads * LANES),
        vmem(*emis.shape),
        vmem(share, width),
        vmem(share, width, dtype=F32),
        vmem(EDGE + 2 * length, width),
        vmem(width, units),
        vmem(width, units),
        vmem(width, units),
        vmem(2 * length, units),
        vmem(spread, 2 * teams, share, block),
        vmem(spread, 2 * teams, share, block),
        vmem(share, width),
        dma((2 * tiles + 4,)),
        dma((3,)),
        dma((3, spread, 3)),
        dma((3, spread)),
        dma((2,)),
        dma((2,)),
        dma((team,)),
        dma((team,)),
        dma((2 * team, 2, 1 + teams)),
        dma((2 * team, 2)),
        dma((2,)),
        dma((spread, 2 * teams)),
        dma((spread, 2 * teams)),
        dma((spread, 2 * teams)),
        dma((spread, 2 * teams)),
        dma((spread,)),
    ]
    return pl.pallas_call(
        functools.partial(step_kernel, first),
        in_specs=[anywhere] * 11 + [inside] * 4,
        out_specs=anywhere,
        out_shape=jax.ShapeDtypeStruct((share, width), BF16),
        scratch_shapes=scratch,
        compiler_params=pltpu.CompilerParams(
            collective_id=1, has_side_effects=True, vmem_limit_bytes=67043328
        ),
        cost_estimate=pl.CostEstimate(flops=10**11, bytes_accessed=10**8, transcendentals=0),
    )(q1, k1, q2, k2, v, valve, emis, skip, gate, up, narrow, gb, coef, norm, taps)


def per_device(
    arriving_hidden_state,
    former_request_vectors,
    former_match_vectors,
    latter_request_vectors,
    latter_match_vectors,
    stored_vectors_both,
    closing_valve_operands,
    update_level_before_squash,
    fading_data_input,
    sparse_fading_boost,
    unitwise_fading_loglevel,
    fading_constant_term,
    unitwise_normalizer_coef,
    emission_map_weights,
    channel_normalizer_coef,
    switching_channel_map,
    broadening_channel_map,
    timewise_convolve_tapvalues,
    narrowing_map_weights_in,
):
    length = former_request_vectors.shape[0]
    level = (
        -jnp.exp(unitwise_fading_loglevel)[..., None]
        * jax.nn.softplus(fading_data_input + fading_constant_term[..., None])
        + sparse_fading_boost
    )
    beta_rate = jax.nn.sigmoid(update_level_before_squash.astype(jnp.float32))
    gates_beta = jnp.concatenate([level, beta_rate], axis=0).reshape(-1, length)
    gates_beta = jnp.pad(gates_beta, ((0, -gates_beta.shape[0] % 8), (0, 0)))
    spare = -latter_request_vectors.shape[1] % LANES
    return whole_step(
        former_request_vectors.shape[1] // LANES,
        former_request_vectors,
        former_match_vectors,
        jnp.pad(latter_request_vectors, ((0, 0), (0, spare))),
        jnp.pad(latter_match_vectors, ((0, 0), (0, spare))),
        stored_vectors_both,
        closing_valve_operands,
        emission_map_weights,
        arriving_hidden_state,
        switching_channel_map,
        broadening_channel_map,
        narrowing_map_weights_in,
        gates_beta,
        unitwise_normalizer_coef.reshape(1, -1),
        channel_normalizer_coef.reshape(1, -1),
        timewise_convolve_tapvalues.astype(F32).reshape(2 * TAPS, -1),
    )


def solution(mesh):
    placed = (
        P(("sp", "tp"), None),
        P("sp", "tp"),
        P("sp", "tp"),
        P("sp", "tp"),
        P("sp", "tp"),
        P("sp", None, "tp"),
        P("sp", None, "tp"),
        P(None, "tp", "sp"),
        P(None, "tp", "sp"),
        P(None, "tp", "sp"),
        P(None, "tp"),
        P(None, "tp"),
        P(),
        P(),
        P(),
        P("sp", "tp"),
        P("sp", "tp"),
        P(None, None, "tp"),
        P("sp", "tp"),
    )
    return jax.shard_map(
        per_device, mesh=mesh, in_specs=placed, out_specs=P(("sp", "tp"), None), check_vma=False
    )
```
